32 devices in a mesh: grp: 2 (over y), kv: 4 (over z), tp: 4 (over x, core).
Axes of the slice: x: 2, y: 2, z: 4, core: 2. Of those that a mesh axis runs over, the one named last changes fastest.
Arguments:
- tokens: bfloat16 [48, 4096], P('grp', ('kv', 'tp')), parts along dimension 0, may hold values from -12 to 12
- lengths: int32 [48], P('grp'), parts along dimension 0, may hold values from 1 to 128, 1536 in all
- attn_gain: float32 [4096], P('kv'), may hold values from 0.1 to 1.9
- w_query: bfloat16 [4096, 4096], P('kv', 'tp'), may hold values from -0.09375 to 0.09375
- w_key: bfloat16 [4096, 4096], P('kv', 'tp'), may hold values from -0.09375 to 0.09375
- w_value: bfloat16 [4096, 4096], P('kv', 'tp'), may hold values from -0.09375 to 0.09375
- w_gate: bfloat16 [4096, 4096], P('kv', 'tp'), may hold values from -0.09375 to 0.09375
- log_decay: float32 [16], P('tp'), may hold values from -1 to 0
- key_cache: bfloat16 [48, 128, 4096], P('grp', 'kv', 'tp'), parts along dimension 0, may hold values from -6 to 6
- value_cache: bfloat16 [48, 128, 4096], P('grp', 'kv', 'tp'), parts along dimension 0, may hold values from -6 to 6
- gn_gain: float32 [4096], P('tp'), may hold values from 0.1 to 1.9
- w_out: bfloat16 [4096, 4096], P('tp', 'kv'), may hold values from -0.1875 to 0.1875
- ffn_gain: float32 [4096], P('kv'), may hold values from 0.1 to 1.9
- w_ffn_gate: bfloat16 [4096, 11264], P('kv', 'tp'), may hold values from -0.09375 to 0.09375
- w_ffn_up: bfloat16 [4096, 11264], P('kv', 'tp'), may hold values from -0.09375 to 0.09375
- w_ffn_down: bfloat16 [11264, 4096], P('tp', 'kv'), may hold values from -0.109375 to 0.109375
Outputs:
- layer_out: bfloat16 [48, 4096], P('grp', ('kv', 'tp')), parts along dimension 0
The draws below stay inside these ranges and needn't reach their ends.
There are 2 independent parts, one for each index of `grp`. The reference program is written for one: setup_inputs(seed, part) draws one part's arguments, and reference() takes and returns one part's arrays. A program takes and returns all parts, laid end to end along the dimension named above; an argument that names none is the same for every part. Nothing has to cross between parts.
All inputs are finite; a program needn't handle non-finite values.
Results may differ from the reference program's by a relative error of at most 0.012.
Values may be sent and summed in bfloat16 or wider, within the bound.
A program may use at most 64 MiB of HBM per device.

```python
import math
import jax
import jax.numpy as jnp
import numpy as np
from jax import lax

HEADS = 16
DK = 256
FF = 11264
SEQS = 24
D = 4096
L_CACHE = 128
N_KV = 4


def draw_tokens(key, part):
    folded = jax.random.fold_in(key, 11)
    second_key = jax.random.fold_in(folded, 0)
    ramp = jnp.arange(N_KV, dtype=jnp.float32) / (N_KV - 1)
    block_scale = jnp.exp(ramp * 1.0986)
    entries = jnp.clip(jax.random.normal(second_key, (SEQS, D), jnp.float32), -4.0, 4.0)
    col_scale = jnp.repeat(block_scale, D // N_KV)
    return (entries * col_scale[None, :]).astype(jnp.bfloat16)


def draw_log_decay(key, part):
    folded = jax.random.fold_in(key, 23)
    pick_key, slow_key, fast_key = jax.random.split(folded, 3)
    slow_share = 0.5
    picked = jax.random.uniform(pick_key, (HEADS,), jnp.float32) < slow_share
    slow_rate = -2.3 * jax.random.uniform(slow_key, (HEADS,), jnp.float32, 0.3, 1.0) / L_CACHE
    fast_rate = -1.0 / jax.random.uniform(fast_key, (HEADS,), jnp.float32, 30.0, 60.0)
    return jnp.where(picked, slow_rate, fast_rate).astype(jnp.float32)


def levels(rng, dims, cuts, smallest, top_value):
    gain = 1.0
    for dim, parts in cuts:
        heights = jax.random.uniform(jax.random.fold_in(jax.random.fold_in(rng, 6), dim), (parts,), jnp.float32, smallest / len(cuts), top_value / len(cuts))
        gain = gain * jnp.repeat(jnp.exp(heights), dims[dim] // parts).reshape((-1,) + (1,) * (len(dims) - 1 - dim))
    return gain


def split_up(count, total, limit, skew):
    portions = [(1 << 20) // math.isqrt(rank ** skew) + 1 for rank in range(2, count + 1)]
    spare, holding = total - limit - (count - 1), [1] * (count - 1)
    while spare > 0:
        free = [i for i in range(count - 1) if holding[i] < limit]
        pool, left = sum([portions[i] for i in free]), spare
        for i in free:
            more = min(limit - holding[i], max(1, left * portions[i] // pool), spare)
            holding[i] = holding[i] + more
            spare = spare - more
    return np.array([limit] + holding)


def uneven_parts(key, count, total, reach, slope):
    if count == 2:
        one = jax.random.randint(key, (), max(1, total - reach), min(reach, total - 1) + 1)
        return jnp.stack([one, total - one])
    sizes = jnp.asarray(split_up(count, total, reach, slope), jnp.int32)
    twos = (count - 1) // 2
    giver, taker = sizes[1:1 + 2 * twos:2], sizes[2:2 + 2 * twos:2]
    margin = jnp.minimum(giver - 1, reach - taker)
    moved = jax.random.randint(jax.random.fold_in(key, 1), (twos,), 0, 1 << 20) % (margin + 1)
    sizes = sizes.at[1:1 + 2 * twos:2].set(giver - moved).at[2:2 + 2 * twos:2].set(taker + moved)
    return sizes[jax.random.permutation(jax.random.fold_in(key, 2), count)]


def centred(stream_key, shape, scale, limit, pieces=(), kind=jnp.bfloat16):
    array = scale * jax.random.normal(stream_key, shape, jnp.float32)
    if pieces:
        array = array * levels(stream_key, shape, pieces, -0.22, 0.18)
    return jnp.clip(array, -limit, limit).astype(kind)


def setup_inputs(seed: int = 0, part: int = 0) -> dict:
    splits = jax.random.split(jax.random.key(seed), 17)
    own_keys = jax.random.split(jax.random.fold_in(splits[16], part), 17)
    return {
        "tokens": draw_tokens(jax.random.fold_in(jax.random.fold_in(splits[16], part), 71), part),
        "lengths": uneven_parts(own_keys[1], SEQS, SEQS * L_CACHE // 2, L_CACHE, 2).astype(jnp.int32),
        "attn_gain": jnp.clip(1.0 + 0.18 * jax.random.normal(splits[2], (D,), jnp.float32), 0.1, 1.9),
        "w_query": centred(splits[3], (D, D), D ** -0.5, 0.09375, ((0, 4), (1, 4))),
        "w_key": centred(splits[4], (D, D), D ** -0.5, 0.09375, ((0, 4), (1, 4))),
        "w_value": centred(splits[5], (D, D), D ** -0.5, 0.09375, ((0, 4), (1, 4))),
        "w_gate": centred(splits[6], (D, D), D ** -0.5, 0.09375, ((0, 4), (1, 4))),
        "log_decay": draw_log_decay(jax.random.fold_in(splits[16], 71), part),
        "key_cache": centred(own_keys[8], (SEQS, L_CACHE, D), 1.0, 6.0, ((1, 4), (2, 4))),
        "value_cache": centred(own_keys[9], (SEQS, L_CACHE, D), 1.0, 6.0, ((1, 4), (2, 4))),
        "gn_gain": jnp.clip(1.0 + 0.18 * jax.random.normal(splits[10], (D,), jnp.float32), 0.1, 1.9),
        "w_out": centred(splits[11], (D, D), (D // 4) ** -0.5, 0.1875, ((0, 4), (1, 4))),
        "ffn_gain": jnp.clip(1.0 + 0.18 * jax.random.normal(splits[12], (D,), jnp.float32), 0.1, 1.9),
        "w_ffn_gate": centred(splits[13], (D, FF), D ** -0.5, 0.09375, ((0, 4), (1, 4))),
        "w_ffn_up": centred(splits[14], (D, FF), D ** -0.5, 0.09375, ((0, 4), (1, 4))),
        "w_ffn_down": centred(splits[15], (FF, D), (FF // 4) ** -0.5, 0.109375, ((0, 4), (1, 4))),
    }


RMS_EPS = 0.1
GN_EPS = 1.0
ROPE_BASE = 10000.0

def rotate(vectors, positions):
    half_dim = vectors.shape[-1] // 2
    inverse = ROPE_BASE ** (-jnp.arange(half_dim, dtype=jnp.float32) / half_dim)
    angles = positions[:, None, None] * inverse[None, None, :]
    cosine = jnp.cos(angles)
    sine_part = jnp.sin(angles)
    front_part = vectors[..., :half_dim]
    back_part = vectors[..., half_dim:]
    return jnp.concatenate([front_part * cosine - back_part * sine_part, front_part * sine_part + back_part * cosine], axis=-1)

def group_norm(totals, gn_gain):
    width = totals.shape[-1]
    center = lax.optimization_barrier(jnp.sum(totals, axis=-1, keepdims=True)) / width
    spread = lax.optimization_barrier(jnp.sum(totals * totals, axis=-1, keepdims=True)) / width - center * center
    normed = (totals - center) * lax.rsqrt(spread + GN_EPS)
    return normed.reshape(normed.shape[0], -1) * gn_gain

def reference(tokens, lengths, attn_gain, w_query, w_key, w_value, w_gate, log_decay, key_cache, value_cache, gn_gain, w_out, ffn_gain, w_ffn_gate, w_ffn_up, w_ffn_down):
    batch_rows = tokens.shape[0]
    heads_all = log_decay.shape[0]
    widened = tokens.astype(jnp.float32)
    factor = lax.rsqrt(lax.optimization_barrier(jnp.sum(widened * widened, axis=1)) / D + RMS_EPS)[:, None]
    scaled = (widened * attn_gain).astype(jnp.bfloat16)
    queries = jnp.dot(scaled, w_query, preferred_element_type=jnp.float32) * factor
    new_keys = jnp.dot(scaled, w_key, preferred_element_type=jnp.float32) * factor
    new_values = jnp.dot(scaled, w_value, preferred_element_type=jnp.float32) * factor
    gates = jnp.dot(scaled, w_gate, preferred_element_type=jnp.float32) * factor
    positions = lengths.astype(jnp.float32)
    queries = rotate(queries.reshape(batch_rows, heads_all, DK), positions) * DK ** (-0.5)
    new_keys = rotate(new_keys.reshape(batch_rows, heads_all, DK), positions)
    new_values = new_values.reshape(batch_rows, heads_all, DK)
    query_low = queries.astype(jnp.bfloat16)
    cache_len = key_cache.shape[1]
    slots = jnp.arange(cache_len, dtype=jnp.int32)

    def one_sequence(packed):
        keys_seq, values_seq, query_seq, length = packed
        keys_wide = keys_seq.astype(jnp.float32).reshape(cache_len, heads_all, DK)
        scores = jnp.einsum('phd,hd->ph', keys_wide, query_seq.astype(jnp.float32))
        gaps = (length - slots).astype(jnp.float32)
        decays = jnp.exp(log_decay[None, :] * jnp.maximum(gaps, 0.0)[:, None])
        mixing = jnp.where((slots < length)[:, None], scores * decays, 0.0).astype(jnp.bfloat16)
        values_wide = values_seq.astype(jnp.float32).reshape(cache_len, heads_all, DK)
        return jnp.einsum('ph,phd->hd', mixing.astype(jnp.float32), values_wide)
    cached = lax.map(one_sequence, (key_cache, value_cache, query_low, lengths.astype(jnp.int32)))
    own_term = lax.optimization_barrier(jnp.sum(queries * new_keys, axis=-1, keepdims=True)) * new_values
    normed = group_norm(cached + own_term, gn_gain)
    gated = (jax.nn.silu(gates) * normed).astype(jnp.bfloat16)
    mixed = jnp.dot(gated, w_out, preferred_element_type=jnp.float32)
    resid = (widened + mixed).astype(jnp.bfloat16)
    resid_wide = resid.astype(jnp.float32)
    factor_mid = lax.rsqrt(lax.optimization_barrier(jnp.sum(resid_wide * resid_wide, axis=1)) / D + RMS_EPS)[:, None]
    scaled_mid = (resid_wide * ffn_gain).astype(jnp.bfloat16)
    gate_mid = jnp.dot(scaled_mid, w_ffn_gate, preferred_element_type=jnp.float32) * factor_mid
    up_mid = jnp.dot(scaled_mid, w_ffn_up, preferred_element_type=jnp.float32) * factor_mid
    hidden = (jax.nn.silu(gate_mid) * up_mid).astype(jnp.bfloat16)
    down = jnp.dot(hidden, w_ffn_down, preferred_element_type=jnp.float32)
    return (resid_wide + down).astype(jnp.bfloat16)
```

```python
import functools
import math

import jax
import jax.numpy as jnp
from jax import lax
from jax.experimental import pallas as pl
from jax.experimental.pallas import tpu as pltpu
from jax.sharding import PartitionSpec as P

DK = 256
D = 4096


RMS_EPS = 0.1
GN_EPS = 1.0
ROPE_BASE = 10000.0


def rotate(vectors, positions):
    half_dim = vectors.shape[-1] // 2
    inverse = ROPE_BASE ** (-jnp.arange(half_dim, dtype=jnp.float32) / half_dim)
    angles = positions[:, None, None] * inverse[None, None, :]
    cosine = jnp.cos(angles)
    sine_part = jnp.sin(angles)
    front_part = vectors[..., :half_dim]
    back_part = vectors[..., half_dim:]
    return jnp.concatenate(
        [front_part * cosine - back_part * sine_part, front_part * sine_part + back_part * cosine],
        axis=-1,
    )


def group_norm(totals, gn_gain):
    width = totals.shape[-1]
    center = jnp.sum(totals, axis=-1, keepdims=True) / width
    spread = jnp.sum(totals * totals, axis=-1, keepdims=True) / width - center * center
    normed = (totals - center) * lax.rsqrt(spread + GN_EPS)
    return normed.reshape(normed.shape[0], -1) * gn_gain


def channel_stat(own_squares):
    return lax.psum(own_squares, "kv")


def input_stat(own_squares):
    return lax.psum(own_squares, "kv")


def cache_partial(query_low, lengths, log_decay, key_cache, value_cache, heads_here):
    batch_rows = query_low.shape[0]
    span = key_cache.shape[1]
    slots = lax.axis_index("kv") * span + jnp.arange(span, dtype=jnp.int32)
    live = slots[None, :] < lengths[:, None]
    gaps = jnp.maximum((lengths[:, None] - slots[None, :]).astype(jnp.float32), 0.0)
    decays = jnp.exp(log_decay[None, None, :] * gaps[:, :, None])
    keys_here = key_cache.reshape(batch_rows, span, heads_here, DK)
    values_here = value_cache.reshape(batch_rows, span, heads_here, DK)
    scores = jnp.einsum("bphd,bhd->bph", keys_here, query_low, preferred_element_type=jnp.float32)
    mixing = jnp.where(live[:, :, None], scores * decays, 0.0).astype(jnp.bfloat16)
    return jnp.einsum("bph,bphd->bhd", mixing, values_here, preferred_element_type=jnp.float32)


def local(
    tokens,
    lengths,
    attn_gain,
    w_query,
    w_key,
    w_value,
    w_gate,
    log_decay,
    key_cache,
    value_cache,
    gn_gain,
    w_out,
    ffn_gain,
    w_ffn_gate,
    w_ffn_up,
    w_ffn_down,
):
    batch_rows = tokens.shape[0]
    heads_here = log_decay.shape[0]
    row_block = lax.all_gather(tokens, "tp", axis=1, tiled=True)
    widened = row_block.astype(jnp.float32)
    own_squares = jnp.sum(widened * widened, axis=1)
    scaled = (widened * attn_gain).astype(jnp.bfloat16)
    part_query = jnp.dot(scaled, w_query, preferred_element_type=jnp.float32)
    part_key = jnp.dot(scaled, w_key, preferred_element_type=jnp.float32)
    part_value = jnp.dot(scaled, w_value, preferred_element_type=jnp.float32)
    part_gate = jnp.dot(scaled, w_gate, preferred_element_type=jnp.float32)
    positions = lengths.astype(jnp.float32)
    total_squares = input_stat(own_squares)
    queries, new_keys, new_values, gates = lax.psum(
        (part_query, part_key, part_value, part_gate), "kv"
    )
    factor = lax.rsqrt(total_squares / D + RMS_EPS)[:, None]
    queries = rotate((queries * factor).reshape(batch_rows, heads_here, DK), positions) * DK ** (
        -0.5
    )
    new_keys = rotate((new_keys * factor).reshape(batch_rows, heads_here, DK), positions)
    new_values = (new_values * factor).reshape(batch_rows, heads_here, DK)
    gates = gates * factor
    query_low = queries.astype(jnp.bfloat16)
    partial_value = cache_partial(query_low, lengths, log_decay, key_cache, value_cache, heads_here)
    cached = lax.psum(partial_value.reshape(batch_rows, heads_here * DK), "kv")
    own_term = jnp.sum(queries * new_keys, axis=-1, keepdims=True) * new_values
    normed = group_norm(cached.reshape(batch_rows, heads_here, DK) + own_term, gn_gain)
    gated = (jax.nn.silu(gates) * normed).astype(jnp.bfloat16)
    out_partial = jnp.dot(gated, w_out, preferred_element_type=jnp.float32)
    mixed = lax.psum_scatter(out_partial, "tp", scatter_dimension=1, tiled=True)
    resid = (tokens.astype(jnp.float32) + mixed).astype(jnp.bfloat16)
    resid_block = lax.all_gather(resid, "tp", axis=1, tiled=True).astype(jnp.float32)
    mid_squares = jnp.sum(resid_block * resid_block, axis=1)
    scaled_mid = (resid_block * ffn_gain).astype(jnp.bfloat16)
    gate_part = jnp.dot(scaled_mid, w_ffn_gate, preferred_element_type=jnp.float32)
    up_part = jnp.dot(scaled_mid, w_ffn_up, preferred_element_type=jnp.float32)
    total_mid = channel_stat(mid_squares)
    gate_sum, up_sum = lax.psum((gate_part, up_part), "kv")
    factor_mid = lax.rsqrt(total_mid / D + RMS_EPS)[:, None]
    hidden = (jax.nn.silu(gate_sum * factor_mid) * (up_sum * factor_mid)).astype(jnp.bfloat16)
    down_partial = jnp.dot(hidden, w_ffn_down, preferred_element_type=jnp.float32)
    down = lax.psum_scatter(down_partial, "tp", scatter_dimension=1, tiled=True)
    return (resid.astype(jnp.float32) + down).astype(jnp.bfloat16)


LANES = 128
F32 = jnp.float32
BF16 = jnp.bfloat16


def window_start(index, tiles, width, parts):
    return (index * (tiles - width) + (parts - 1) // 2) // (parts - 1)


def layer_kernel(
    n_kv,
    n_tp,
    tokens_ref,
    lengths_ref,
    attn_gain_ref,
    log_decay_ref,
    gn_gain_ref,
    ffn_gain_ref,
    wq_hbm,
    wk_hbm,
    wv_hbm,
    wg_hbm,
    kc_hbm,
    vc_hbm,
    wo_hbm,
    wfg_hbm,
    wfu_hbm,
    wfd_hbm,
    out_ref,
    wq,
    wk,
    wv,
    wg,
    kc,
    vc,
    wo,
    wfg,
    wfu,
    wfd,
    tok_buf,
    x_buf,
    sq_send,
    sq_recv,
    q_send,
    q_recv,
    q_full,
    trig,
    decay_buf,
    kvg_send,
    kvg_recv,
    cached_buf,
    ca_send,
    ca_recv,
    gt_buf,
    o_buf,
    resid_buf,
    sqm_send,
    sqm_recv,
    gu_send,
    gu_recv,
    hid_buf,
    down_buf,
    d_send,
    d_recv,
    load_sem,
    kv_send_sem,
    kv_recv_sem,
    tp_send_sem,
    tp_recv_sem,
):
    rows, own_cols = tokens_ref.shape
    depth, wide = wq.shape
    span = kc.shape[1]
    half = DK // 2
    tiles = wfg.shape[1] // LANES
    win = hid_buf.shape[2]
    me_kv = lax.axis_index("kv")
    me_tp = lax.axis_index("tp")

    def kv_peer(j):
        return lax.rem(me_kv + j, n_kv)

    def kv_from(j):
        return lax.rem(me_kv + n_kv - j, n_kv)

    def tp_peer(j):
        return lax.rem(me_tp + j, n_tp)

    def tp_from(j):
        return lax.rem(me_tp + n_tp - j, n_tp)

    loads = {}
    for slot, (name, src, dst) in enumerate(
        (
            ("wq", wq_hbm, wq),
            ("kc", kc_hbm, kc),
            ("vc", vc_hbm, vc),
            ("wk", wk_hbm, wk),
            ("wv", wv_hbm, wv),
            ("wg", wg_hbm, wg),
            ("wo", wo_hbm, wo),
            ("wfg", wfg_hbm, wfg),
            ("wfu", wfu_hbm, wfu),
            ("wfd", wfd_hbm, wfd),
        )
    ):
        loads[name] = pltpu.make_async_copy(src, dst, load_sem.at[slot])

    sent = []

    def to_kv(phase, j, src, dst):
        copy = pltpu.make_async_remote_copy(
            src_ref=src,
            dst_ref=dst,
            send_sem=kv_send_sem.at[phase, j],
            recv_sem=kv_recv_sem.at[phase, j],
            device_id={"kv": kv_peer(j)},
            device_id_type=pl.DeviceIdType.MESH,
        )
        copy.start()
        sent.append(copy)
        return copy

    def to_tp(phase, j, src, dst):
        copy = pltpu.make_async_remote_copy(
            src_ref=src,
            dst_ref=dst,
            send_sem=tp_send_sem.at[phase, j],
            recv_sem=tp_recv_sem.at[phase, j],
            device_id={"tp": tp_peer(j)},
            device_id_type=pl.DeviceIdType.MESH,
        )
        copy.start()
        sent.append(copy)
        return copy

    loads["wq"].start()

    barrier = pltpu.get_barrier_semaphore()
    for j in range(1, n_kv):
        pl.semaphore_signal(
            barrier, inc=1, device_id={"kv": kv_peer(j)}, device_id_type=pl.DeviceIdType.MESH
        )
    for j in range(1, n_tp):
        pl.semaphore_signal(
            barrier, inc=1, device_id={"tp": tp_peer(j)}, device_id_type=pl.DeviceIdType.MESH
        )
    for name in ("kc", "wk", "wv", "wg", "vc"):
        loads[name].start()
    pl.semaphore_wait(barrier, n_kv + n_tp - 2)

    tok_copies = [to_tp(0, j, tokens_ref, tok_buf.at[me_tp]) for j in range(1, n_tp)]
    tok_buf[me_tp] = tokens_ref[...]

    row_id = lax.broadcasted_iota(jnp.int32, (rows, LANES), 0)
    lens = jnp.zeros((rows, LANES), jnp.int32)
    for b in range(rows):
        lens = jnp.where(row_id == b, lengths_ref[b], lens)
    lane = lax.broadcasted_iota(jnp.int32, (rows, half), 1).astype(F32)
    inverse = jnp.exp(lane * (-math.log(ROPE_BASE) / half))
    angles = lens[:, :1].astype(F32) * inverse
    trig[0] = jnp.cos(angles)
    trig[1] = jnp.sin(angles)
    places = rows * span
    col = lax.broadcasted_iota(jnp.int32, (rows, places), 1)
    row = lax.broadcasted_iota(jnp.int32, (rows, places), 0)
    slot = col - row * span
    position = slot + me_kv * span
    gap = lens[:, :1] - position
    live = (slot >= 0) & (slot < span) & (gap > 0)
    gap_f = jnp.where(live, gap, 0).astype(F32)
    for h in range(n_kv):
        decay_buf[h] = jnp.where(live, jnp.exp(gap_f * log_decay_ref[h]), 0.0)

    def rotate_in(front, back):
        cosine, sine = trig[0], trig[1]
        return front * cosine - back * sine, front * sine + back * cosine

    for copy in tok_copies:
        copy.wait_recv()
    squares = jnp.zeros((rows, 1), F32)
    for c in range(n_tp):
        wide_tok = tok_buf[c].astype(F32)
        squares = squares + jnp.sum(wide_tok * wide_tok, axis=1, keepdims=True)
        cols = pl.ds(c * own_cols, own_cols)
        x_buf[:, cols] = (wide_tok * attn_gain_ref[:, cols]).astype(BF16)
    sq_send[...] = jnp.broadcast_to(squares, (rows, LANES))
    sq_copies = [to_kv(0, j, sq_send, sq_recv.at[j]) for j in range(1, n_kv)]

    x = x_buf[...]
    loads["wq"].wait()
    q_own = jnp.dot(x, wq[...], preferred_element_type=F32)
    q_send[...] = q_own.astype(BF16)
    q_full[...] = q_own
    q_copies = [to_kv(1, j, q_send, q_recv.at[j]) for j in range(1, n_kv)]
    for name in ("wo", "wfg", "wfu", "wfd"):
        loads[name].start()

    for name in ("wk", "wv", "wg"):
        loads[name].wait()
    kvg_copies = []
    own_kvg = []
    for j in tuple(range(1, n_kv)) + (0,):
        cols = pl.ds(pl.multiple_of(kv_peer(j) * DK, DK), DK)
        for i, weight in enumerate((wk, wv, wg)):
            part = jnp.dot(x, weight[:, cols], preferred_element_type=F32)
            if j:
                kvg_send[j, :, pl.ds(i * DK, DK)] = part.astype(BF16)
            else:
                own_kvg.append(part)
        if j:
            kvg_copies.append(to_kv(2, j, kvg_send.at[j], kvg_recv.at[j]))

    for copy in sq_copies:
        copy.wait_recv()
    total_sq = sq_send[...]
    for j in range(1, n_kv):
        total_sq = total_sq + sq_recv[j]
    factor = lax.rsqrt(total_sq / D + RMS_EPS)[:, :1]

    for copy in q_copies:
        copy.wait_recv()
    loads["kc"].wait()
    loads["vc"].wait()
    for h in range(n_kv):
        halves = []
        for lo in (h * DK, h * DK + half):
            cols = pl.ds(lo, half)
            piece = q_full[:, cols]
            for j in range(1, n_kv):
                piece = piece + q_recv[j, :, cols].astype(F32)
            halves.append(piece * factor)
        front, back = rotate_in(*halves)
        q_full[:, pl.ds(h * DK, half)] = front * DK ** (-0.5)
        q_full[:, pl.ds(h * DK + half, half)] = back * DK ** (-0.5)
        cols = pl.ds(h * DK, DK)
        keys = kc[:, :, cols].reshape(places, DK)
        scores = lax.dot_general(
            q_full[:, cols].astype(BF16),
            keys,
            (((1,), (1,)), ((), ())),
            preferred_element_type=F32,
        )
        mixing = (scores * decay_buf[h]).astype(BF16)
        values = vc[:, :, cols].reshape(places, DK)
        cached_buf[:, cols] = jnp.dot(mixing, values, preferred_element_type=F32)
    ca_copies = []
    for j in range(1, n_kv):
        cols = pl.ds(pl.multiple_of(kv_peer(j) * DK, DK), DK)
        ca_send[j] = cached_buf[:, cols].astype(BF16)
        ca_copies.append(to_kv(3, j, ca_send.at[j], ca_recv.at[j]))

    for copy in kvg_copies:
        copy.wait_recv()
    own_head = pl.ds(pl.multiple_of(me_kv * DK, DK), DK)
    summed = []
    for i in range(3):
        piece = own_kvg[i]
        for j in range(1, n_kv):
            piece = piece + kvg_recv[j, :, pl.ds(i * DK, DK)].astype(F32)
        summed.append(piece * factor)
    new_key, new_value, gate = summed
    front, back = rotate_in(new_key[:, :half], new_key[:, half:])
    query = q_full[:, own_head]
    score = jnp.sum(query[:, :half] * front + query[:, half:] * back, axis=1, keepdims=True)
    own_term = score * new_value
    gate = gate / (1.0 + jnp.exp(-gate))
    totals = own_term + cached_buf[:, own_head]
    for copy in ca_copies:
        copy.wait_recv()
    for j in range(1, n_kv):
        totals = totals + ca_recv[j].astype(F32)
    center = jnp.sum(totals, axis=1, keepdims=True) / DK
    spread = jnp.sum(totals * totals, axis=1, keepdims=True) / DK - center * center
    normed = (totals - center) * lax.rsqrt(spread + GN_EPS) * gn_gain_ref[:, own_head]
    gt_buf[me_kv] = (gate * normed).astype(BF16)
    gt_copies = [to_kv(4, j, gt_buf.at[me_kv], gt_buf.at[me_kv]) for j in range(1, n_kv)]

    loads["wo"].wait()
    for copy in gt_copies:
        copy.wait_recv()
    for c in range(n_kv):
        x_buf[:, pl.ds(c * DK, DK)] = gt_buf[c]
    o_buf[me_tp] = jnp.dot(x_buf[...], wo[...], preferred_element_type=F32).astype(BF16)
    o_copies = [to_tp(1, j, o_buf.at[me_tp], o_buf.at[me_tp]) for j in range(1, n_tp)]
    for copy in o_copies:
        copy.wait_recv()
    squares = jnp.zeros((rows, 1), F32)
    for c in range(n_tp):
        cols = pl.ds(c * own_cols, own_cols)
        mixed = o_buf[0, :, cols].astype(F32)
        for t in range(1, n_tp):
            mixed = mixed + o_buf[t, :, cols].astype(F32)
        resid = (tok_buf[c].astype(F32) + mixed).astype(BF16)
        resid_wide = resid.astype(F32)
        resid_buf[c] = resid_wide
        squares = squares + jnp.sum(resid_wide * resid_wide, axis=1, keepdims=True)
        x_buf[:, cols] = (resid_wide * ffn_gain_ref[:, cols]).astype(BF16)
    sqm_send[...] = jnp.broadcast_to(squares, (rows, LANES))
    sqm_copies = [to_kv(5, j, sqm_send, sqm_recv.at[j]) for j in range(1, n_kv)]

    x = x_buf[...]
    loads["wfg"].wait()
    loads["wfu"].wait()
    gu_copies = []
    own_gu = []
    for j in tuple(range(1, n_kv)) + (0,):
        start = window_start(kv_peer(j), tiles, win // LANES, n_kv)
        cols = pl.ds(pl.multiple_of(start * LANES, LANES), win)
        for i, weight in enumerate((wfg, wfu)):
            part = jnp.dot(x, weight[:, cols], preferred_element_type=F32)
            if j:
                gu_send[j, :, pl.ds(i * win, win)] = part.astype(BF16)
            else:
                own_gu.append(part)
        if j:
            gu_copies.append(to_kv(6, j, gu_send.at[j], gu_recv.at[j]))

    for copy in sqm_copies:
        copy.wait_recv()
    total_sq = sqm_send[...]
    for j in range(1, n_kv):
        total_sq = total_sq + sqm_recv[j]
    factor = lax.rsqrt(total_sq / D + RMS_EPS)[:, :1]
    for copy in gu_copies:
        copy.wait_recv()
    summed = []
    for i in range(2):
        piece = own_gu[i]
        for j in range(1, n_kv):
            piece = piece + gu_recv[j, :, pl.ds(i * win, win)].astype(F32)
        summed.append(piece * factor)
    gate, up = summed
    hidden = gate / (1.0 + jnp.exp(-gate)) * up
    here = window_start(me_kv, tiles, win // LANES, n_kv)
    after = window_start(me_kv + 1, tiles, win // LANES, n_kv)
    kept = jnp.where(me_kv == n_kv - 1, win, (after - here) * LANES)
    column = lax.broadcasted_iota(jnp.int32, (rows, win), 1)
    hid_buf[me_kv] = jnp.where(column < kept, hidden, 0.0).astype(BF16)
    hid_copies = [to_kv(7, j, hid_buf.at[me_kv], hid_buf.at[me_kv]) for j in range(1, n_kv)]

    loads["wfd"].wait()
    down = None
    for j in range(n_kv):
        if j:
            hid_copies[j - 1].wait_recv()
        source = kv_from(j)
        start = window_start(source, tiles, win // LANES, n_kv)
        weight = wfd[pl.ds(pl.multiple_of(start * LANES, LANES), win), :]
        part = jnp.dot(hid_buf[source], weight, preferred_element_type=F32)
        down = part if down is None else down + part
    down_buf[...] = down
    d_copies = []
    for j in range(1, n_tp):
        cols = pl.ds(pl.multiple_of(tp_peer(j) * own_cols, own_cols), own_cols)
        d_send[j] = down_buf[:, cols].astype(BF16)
        d_copies.append(to_tp(2, j, d_send.at[j], d_recv.at[j]))
    own = pl.ds(pl.multiple_of(me_tp * own_cols, own_cols), own_cols)
    result = down_buf[:, own] + resid_buf[me_tp]
    for j in range(1, n_tp):
        d_copies[j - 1].wait_recv()
        result = result + d_recv[j].astype(F32)
    out_ref[...] = result.astype(BF16)
    for copy in sent:
        copy.wait_send()


def fused(
    n_kv,
    n_tp,
    tokens,
    lengths,
    attn_gain,
    w_query,
    w_key,
    w_value,
    w_gate,
    log_decay,
    key_cache,
    value_cache,
    gn_gain,
    w_out,
    ffn_gain,
    w_ffn_gate,
    w_ffn_up,
    w_ffn_down,
):
    rows, own_cols = tokens.shape
    depth, wide = w_query.shape
    units = w_ffn_gate.shape[1]
    tiles = units // LANES
    win = -(-tiles // n_kv) * LANES
    span = key_cache.shape[1]
    vmem = pl.BlockSpec(memory_space=pltpu.VMEM)
    smem = pl.BlockSpec(memory_space=pltpu.SMEM)
    hbm = pl.BlockSpec(memory_space=pl.ANY)
    streamed = (
        w_query,
        w_key,
        w_value,
        w_gate,
        key_cache,
        value_cache,
        w_out,
        w_ffn_gate,
        w_ffn_up,
        w_ffn_down,
    )
    scratch = [pltpu.VMEM(a.shape, a.dtype) for a in streamed] + [
        pltpu.VMEM((n_tp, rows, own_cols), BF16),
        pltpu.VMEM((rows, depth), BF16),
        pltpu.VMEM((rows, LANES), F32),
        pltpu.VMEM((n_kv, rows, LANES), F32),
        pltpu.VMEM((rows, wide), BF16),
        pltpu.VMEM((n_kv, rows, wide), BF16),
        pltpu.VMEM((rows, wide), F32),
        pltpu.VMEM((2, rows, DK // 2), F32),
        pltpu.VMEM((n_kv, rows, rows * span), F32),
        pltpu.VMEM((n_kv, rows, 3 * DK), BF16),
        pltpu.VMEM((n_kv, rows, 3 * DK), BF16),
        pltpu.VMEM((rows, wide), F32),
        pltpu.VMEM((n_kv, rows, DK), BF16),
        pltpu.VMEM((n_kv, rows, DK), BF16),
        pltpu.VMEM((n_kv, rows, DK), BF16),
        pltpu.VMEM((n_tp, rows, depth), BF16),
        pltpu.VMEM((n_tp, rows, own_cols), F32),
        pltpu.VMEM((rows, LANES), F32),
        pltpu.VMEM((n_kv, rows, LANES), F32),
        pltpu.VMEM((n_kv, rows, 2 * win), BF16),
        pltpu.VMEM((n_kv, rows, 2 * win), BF16),
        pltpu.VMEM((n_kv, rows, win), BF16),
        pltpu.VMEM((rows, depth), F32),
        pltpu.VMEM((n_tp, rows, own_cols), BF16),
        pltpu.VMEM((n_tp, rows, own_cols), BF16),
        pltpu.SemaphoreType.DMA((len(streamed),)),
        pltpu.SemaphoreType.DMA((8, n_kv)),
        pltpu.SemaphoreType.DMA((8, n_kv)),
        pltpu.SemaphoreType.DMA((3, n_tp)),
        pltpu.SemaphoreType.DMA((3, n_tp)),
    ]
    return pl.pallas_call(
        functools.partial(layer_kernel, n_kv, n_tp),
        out_shape=jax.ShapeDtypeStruct((rows, own_cols), BF16),
        in_specs=[vmem, smem, vmem, smem, vmem, vmem] + [hbm] * len(streamed),
        out_specs=vmem,
        scratch_shapes=scratch,
        compiler_params=pltpu.CompilerParams(
            collective_id=0, has_side_effects=True, vmem_limit_bytes=60 * 1024 * 1024
        ),
    )(
        tokens,
        lengths,
        attn_gain[None, :],
        log_decay,
        gn_gain[None, :],
        ffn_gain[None, :],
        *streamed,
    )


def fits(mesh, tokens, log_decay, key_cache, w_query, w_ffn_gate):
    n_kv, n_tp, n_grp = mesh.shape["kv"], mesh.shape["tp"], mesh.shape["grp"]
    heads, span = log_decay.shape[0], key_cache.shape[1] // n_kv
    return (
        n_kv > 1
        and n_tp > 1
        and heads == n_kv * n_tp
        and tokens.shape[1] // n_kv == heads * DK // n_tp
        and tokens.shape[1] % (n_kv * n_tp * LANES) == 0
        and w_ffn_gate.shape[1] % (n_tp * LANES) == 0
        and tokens.shape[0] // n_grp % 8 == 0
        and span % 16 == 0
        and span <= 64
    )


def solution(mesh):
    specs = (
        P("grp", ("kv", "tp")),
        P("grp"),
        P("kv"),
        P("kv", "tp"),
        P("kv", "tp"),
        P("kv", "tp"),
        P("kv", "tp"),
        P("tp"),
        P("grp", "kv", "tp"),
        P("grp", "kv", "tp"),
        P("tp"),
        P("tp", "kv"),
        P("kv"),
        P("kv", "tp"),
        P("kv", "tp"),
        P("tp", "kv"),
    )

    def whole(*arrays):
        tokens, w_query, log_decay, key_cache = arrays[0], arrays[3], arrays[7], arrays[8]
        if fits(mesh, tokens, log_decay, key_cache, w_query, arrays[13]):
            body = functools.partial(fused, mesh.shape["kv"], mesh.shape["tp"])
        else:
            body = local
        return jax.shard_map(
            body,
            mesh=mesh,
            in_specs=specs,
            out_specs=P("grp", ("kv", "tp")),
            check_vma=False,
        )(*arrays)

    return whole
```

```python
import functools
import math

import jax
import jax.numpy as jnp
from jax import lax
from jax.experimental import pallas as pl
from jax.experimental.pallas import tpu as pltpu
from jax.sharding import PartitionSpec as P

DK = 256
D = 4096


RMS_EPS = 0.1
GN_EPS = 1.0
ROPE_BASE = 10000.0


def rotate(vectors, positions):
    half_dim = vectors.shape[-1] // 2
    inverse = ROPE_BASE ** (-jnp.arange(half_dim, dtype=jnp.float32) / half_dim)
    angles = positions[:, None, None] * inverse[None, None, :]
    cosine = jnp.cos(angles)
    sine_part = jnp.sin(angles)
    front_part = vectors[..., :half_dim]
    back_part = vectors[..., half_dim:]
    return jnp.concatenate(
        [front_part * cosine - back_part * sine_part, front_part * sine_part + back_part * cosine],
        axis=-1,
    )


def group_norm(totals, gn_gain):
    width = totals.shape[-1]
    center = jnp.sum(totals, axis=-1, keepdims=True) / width
    spread = jnp.sum(totals * totals, axis=-1, keepdims=True) / width - center * center
    normed = (totals - center) * lax.rsqrt(spread + GN_EPS)
    return normed.reshape(normed.shape[0], -1) * gn_gain


def channel_stat(own_squares):
    return lax.psum(own_squares, "kv")


def input_stat(own_squares):
    return lax.psum(own_squares, "kv")


def cache_partial(query_low, lengths, log_decay, key_cache, value_cache, heads_here):
    batch_rows = query_low.shape[0]
    span = key_cache.shape[1]
    slots = lax.axis_index("kv") * span + jnp.arange(span, dtype=jnp.int32)
    live = slots[None, :] < lengths[:, None]
    gaps = jnp.maximum((lengths[:, None] - slots[None, :]).astype(jnp.float32), 0.0)
    decays = jnp.exp(log_decay[None, None, :] * gaps[:, :, None])
    keys_here = key_cache.reshape(batch_rows, span, heads_here, DK)
    values_here = value_cache.reshape(batch_rows, span, heads_here, DK)
    scores = jnp.einsum("bphd,bhd->bph", keys_here, query_low, preferred_element_type=jnp.float32)
    mixing = jnp.where(live[:, :, None], scores * decays, 0.0).astype(jnp.bfloat16)
    return jnp.einsum("bph,bphd->bhd", mixing, values_here, preferred_element_type=jnp.float32)


def local(
    tokens,
    lengths,
    attn_gain,
    w_query,
    w_key,
    w_value,
    w_gate,
    log_decay,
    key_cache,
    value_cache,
    gn_gain,
    w_out,
    ffn_gain,
    w_ffn_gate,
    w_ffn_up,
    w_ffn_down,
):
    batch_rows = tokens.shape[0]
    heads_here = log_decay.shape[0]
    row_block = lax.all_gather(tokens, "tp", axis=1, tiled=True)
    widened = row_block.astype(jnp.float32)
    own_squares = jnp.sum(widened * widened, axis=1)
    scaled = (widened * attn_gain).astype(jnp.bfloat16)
    part_query = jnp.dot(scaled, w_query, preferred_element_type=jnp.float32)
    part_key = jnp.dot(scaled, w_key, preferred_element_type=jnp.float32)
    part_value = jnp.dot(scaled, w_value, preferred_element_type=jnp.float32)
    part_gate = jnp.dot(scaled, w_gate, preferred_element_type=jnp.float32)
    positions = lengths.astype(jnp.float32)
    total_squares = input_stat(own_squares)
    queries, new_keys, new_values, gates = lax.psum(
        (part_query, part_key, part_value, part_gate), "kv"
    )
    factor = lax.rsqrt(total_squares / D + RMS_EPS)[:, None]
    queries = rotate((queries * factor).reshape(batch_rows, heads_here, DK), positions) * DK ** (
        -0.5
    )
    new_keys = rotate((new_keys * factor).reshape(batch_rows, heads_here, DK), positions)
    new_values = (new_values * factor).reshape(batch_rows, heads_here, DK)
    gates = gates * factor
    query_low = queries.astype(jnp.bfloat16)
    partial_value = cache_partial(query_low, lengths, log_decay, key_cache, value_cache, heads_here)
    cached = lax.psum(partial_value.reshape(batch_rows, heads_here * DK), "kv")
    own_term = jnp.sum(queries * new_keys, axis=-1, keepdims=True) * new_values
    normed = group_norm(cached.reshape(batch_rows, heads_here, DK) + own_term, gn_gain)
    gated = (jax.nn.silu(gates) * normed).astype(jnp.bfloat16)
    out_partial = jnp.dot(gated, w_out, preferred_element_type=jnp.float32)
    mixed = lax.psum_scatter(out_partial, "tp", scatter_dimension=1, tiled=True)
    resid = (tokens.astype(jnp.float32) + mixed).astype(jnp.bfloat16)
    resid_block = lax.all_gather(resid, "tp", axis=1, tiled=True).astype(jnp.float32)
    mid_squares = jnp.sum(resid_block * resid_block, axis=1)
    scaled_mid = (resid_block * ffn_gain).astype(jnp.bfloat16)
    gate_part = jnp.dot(scaled_mid, w_ffn_gate, preferred_element_type=jnp.float32)
    up_part = jnp.dot(scaled_mid, w_ffn_up, preferred_element_type=jnp.float32)
    total_mid = channel_stat(mid_squares)
    gate_sum, up_sum = lax.psum((gate_part, up_part), "kv")
    factor_mid = lax.rsqrt(total_mid / D + RMS_EPS)[:, None]
    hidden = (jax.nn.silu(gate_sum * factor_mid) * (up_sum * factor_mid)).astype(jnp.bfloat16)
    down_partial = jnp.dot(hidden, w_ffn_down, preferred_element_type=jnp.float32)
    down = lax.psum_scatter(down_partial, "tp", scatter_dimension=1, tiled=True)
    return (resid.astype(jnp.float32) + down).astype(jnp.bfloat16)


LANES = 128
F32 = jnp.float32
BF16 = jnp.bfloat16


def window_start(index, tiles, width, parts):
    return (index * (tiles - width) + (parts - 1) // 2) // (parts - 1)


def partner(index, j, parts):
    found, bit = 0, 1
    while bit < parts:
        digit = (index // bit) % 2
        found = found + bit * ((1 - digit) if (j // bit) % 2 else digit)
        bit *= 2
    return found


def pack(value):
    middle = value.shape[1] // 2
    return jnp.concatenate([value[:, :middle], value[:, middle:]], axis=0).astype(BF16)


def unpack(packed):
    wide = packed.astype(F32)
    rows = wide.shape[0] // 2
    return jnp.concatenate([wide[:rows], wide[rows:]], axis=1)


def layer_kernel(
    n_kv,
    n_tp,
    tokens_ref,
    lengths_ref,
    attn_gain_ref,
    log_decay_ref,
    gn_gain_ref,
    ffn_gain_ref,
    wq_hbm,
    wk_hbm,
    wv_hbm,
    wg_hbm,
    kc_hbm,
    vc_hbm,
    wo_hbm,
    wfg_hbm,
    wfu_hbm,
    wfd_hbm,
    out_ref,
    wq,
    wk,
    wv,
    wg,
    kc,
    vc,
    wo,
    wfg,
    wfu,
    wfd,
    tok_buf,
    x_buf,
    sq_send,
    sq_recv,
    q_send,
    q_recv,
    q_full,
    trig,
    decay_buf,
    kvg_send,
    kvg_recv,
    cached_buf,
    ca_send,
    ca_recv,
    gt_buf,
    o_buf,
    resid_buf,
    sqm_send,
    sqm_recv,
    gu_send,
    gu_recv,
    hid_buf,
    down_buf,
    d_send,
    d_recv,
    load_sem,
    kv_send_sem,
    kv_recv_sem,
    tp_send_sem,
    tp_recv_sem,
):
    rows, own_cols = tokens_ref.shape
    depth, wide = wq.shape
    span = kc.shape[1]
    half = DK // 2
    tiles = wfg.shape[1] // LANES
    win = gu_send.shape[2]
    me_kv = lax.axis_index("kv")
    me_tp = lax.axis_index("tp")

    def kv_peer(j):
        return partner(me_kv, j, n_kv)

    def tp_peer(j):
        return partner(me_tp, j, n_tp)

    kv_order = tuple(range(n_kv - 1, 0, -1))
    tp_order = tuple(range(n_tp - 1, 0, -1))

    loads = {}
    for slot, (name, src, dst) in enumerate(
        (
            ("wq", wq_hbm, wq),
            ("kc", kc_hbm, kc),
            ("vc", vc_hbm, vc),
            ("wk", wk_hbm, wk),
            ("wv", wv_hbm, wv),
            ("wg", wg_hbm, wg),
            ("wo", wo_hbm, wo),
            ("wfg", wfg_hbm, wfg),
            ("wfu", wfu_hbm, wfu),
            ("wfd", wfd_hbm, wfd),
        )
    ):
        loads[name] = pltpu.make_async_copy(src, dst, load_sem.at[slot])

    sent = []

    def to_kv(phase, j, src, dst):
        copy = pltpu.make_async_remote_copy(
            src_ref=src,
            dst_ref=dst,
            send_sem=kv_send_sem.at[phase, j],
            recv_sem=kv_recv_sem.at[phase, j],
            device_id={"kv": kv_peer(j)},
            device_id_type=pl.DeviceIdType.MESH,
        )
        copy.start()
        sent.append(copy)
        return copy

    def to_tp(phase, j, src, dst):
        copy = pltpu.make_async_remote_copy(
            src_ref=src,
            dst_ref=dst,
            send_sem=tp_send_sem.at[phase, j],
            recv_sem=tp_recv_sem.at[phase, j],
            device_id={"tp": tp_peer(j)},
            device_id_type=pl.DeviceIdType.MESH,
        )
        copy.start()
        sent.append(copy)
        return copy

    loads["wq"].start()

    barrier = pltpu.get_barrier_semaphore()
    for j in range(1, n_kv):
        pl.semaphore_signal(
            barrier, inc=1, device_id={"kv": kv_peer(j)}, device_id_type=pl.DeviceIdType.MESH
        )
    for j in range(1, n_tp):
        pl.semaphore_signal(
            barrier, inc=1, device_id={"tp": tp_peer(j)}, device_id_type=pl.DeviceIdType.MESH
        )
    pl.semaphore_wait(barrier, n_kv + n_tp - 2)

    tok_copies = [to_tp(0, j, tokens_ref, tok_buf.at[me_tp]) for j in tp_order]
    for name in ("wk", "wv", "wg", "kc", "vc"):
        loads[name].start()
    tok_buf[me_tp] = tokens_ref[...]

    row_id = lax.broadcasted_iota(jnp.int32, (rows, LANES), 0)
    lens = jnp.zeros((rows, LANES), jnp.int32)
    for b in range(rows):
        lens = jnp.where(row_id == b, lengths_ref[b], lens)
    lane = lax.broadcasted_iota(jnp.int32, (rows, half), 1).astype(F32)
    inverse = jnp.exp(lane * (-math.log(ROPE_BASE) / half))
    angles = lens[:, :1].astype(F32) * inverse
    trig[0] = jnp.cos(angles)
    trig[1] = jnp.sin(angles)
    places = rows * span
    col = lax.broadcasted_iota(jnp.int32, (rows, places), 1)
    row = lax.broadcasted_iota(jnp.int32, (rows, places), 0)
    slot = col - row * span
    position = slot + me_kv * span
    gap = lens[:, :1] - position
    live = (slot >= 0) & (slot < span) & (gap > 0)
    gap_f = jnp.where(live, gap, 0).astype(F32)
    for h in range(n_kv):
        decay_buf[h] = jnp.where(live, jnp.exp(gap_f * log_decay_ref[h]), 0.0)

    def rotate_in(front, back):
        cosine, sine = trig[0], trig[1]
        return front * cosine - back * sine, front * sine + back * cosine

    for copy in tok_copies:
        copy.wait_recv()
    squares = jnp.zeros((rows, 1), F32)
    for c in range(n_tp):
        wide_tok = tok_buf[c].astype(F32)
        squares = squares + jnp.sum(wide_tok * wide_tok, axis=1, keepdims=True)
        cols = pl.ds(c * own_cols, own_cols)
        x_buf[:, cols] = (wide_tok * attn_gain_ref[:, cols]).astype(BF16)
    sq_send[...] = jnp.broadcast_to(squares, (rows, LANES))
    sq_copies = [to_kv(0, j, sq_send, sq_recv.at[j]) for j in kv_order]

    x = x_buf[...]
    loads["wq"].wait()
    q_own = jnp.dot(x, wq[...], preferred_element_type=F32)
    q_send[...] = pack(q_own)
    q_full[...] = q_own
    q_copies = [to_kv(1, j, q_send, q_recv.at[j]) for j in kv_order]
    for name in ("wo", "wfg", "wfu", "wfd"):
        loads[name].start()

    for name in ("wk", "wv", "wg"):
        loads[name].wait()
    kvg_copies = []
    for j in kv_order + (0,):
        cols = pl.ds(pl.multiple_of(kv_peer(j) * DK, DK), DK)
        parts = [
            jnp.dot(x, weight[:, cols], preferred_element_type=F32) for weight in (wk, wv, wg)
        ]
        if j:
            kvg_send[j] = pack(jnp.concatenate(parts, axis=1))
            kvg_copies.append(to_kv(2, j, kvg_send.at[j], kvg_recv.at[j]))
        else:
            own_kvg = jnp.concatenate(parts, axis=1)

    for copy in sq_copies:
        copy.wait_recv()
    total_sq = sq_send[...]
    for j in range(1, n_kv):
        total_sq = total_sq + sq_recv[j]
    factor = lax.rsqrt(total_sq / D + RMS_EPS)[:, :1]

    for copy in q_copies:
        copy.wait_recv()
    loads["kc"].wait()
    loads["vc"].wait()
    query = q_full[...]
    for j in kv_order:
        query = query + unpack(q_recv[j])
    query = query * factor
    for h in range(n_kv):
        halves = (query[:, h * DK : h * DK + half], query[:, h * DK + half : (h + 1) * DK])
        front, back = rotate_in(*halves)
        q_full[:, pl.ds(h * DK, half)] = front * DK ** (-0.5)
        q_full[:, pl.ds(h * DK + half, half)] = back * DK ** (-0.5)
        cols = pl.ds(h * DK, DK)
        keys = kc[:, :, cols].reshape(places, DK)
        scores = lax.dot_general(
            q_full[:, cols].astype(BF16),
            keys,
            (((1,), (1,)), ((), ())),
            preferred_element_type=F32,
        )
        mixing = (scores * decay_buf[h]).astype(BF16)
        values = vc[:, :, cols].reshape(places, DK)
        cached_buf[:, cols] = jnp.dot(mixing, values, preferred_element_type=F32)
    ca_copies = []
    for j in kv_order:
        cols = pl.ds(pl.multiple_of(kv_peer(j) * DK, DK), DK)
        ca_send[j] = pack(cached_buf[:, cols])
        ca_copies.append(to_kv(3, j, ca_send.at[j], ca_recv.at[j]))

    for copy in kvg_copies:
        copy.wait_recv()
    own_head = pl.ds(pl.multiple_of(me_kv * DK, DK), DK)
    for j in kv_order:
        own_kvg = own_kvg + unpack(kvg_recv[j])
    own_kvg = own_kvg * factor
    summed = [own_kvg[:, i * DK : (i + 1) * DK] for i in range(3)]
    new_key, new_value, gate = summed
    front, back = rotate_in(new_key[:, :half], new_key[:, half:])
    query = q_full[:, own_head]
    score = jnp.sum(query[:, :half] * front + query[:, half:] * back, axis=1, keepdims=True)
    own_term = score * new_value
    gate = gate / (1.0 + jnp.exp(-gate))
    totals = own_term + cached_buf[:, own_head]
    for copy in ca_copies:
        copy.wait_recv()
    for j in range(1, n_kv):
        totals = totals + unpack(ca_recv[j])
    center = jnp.sum(totals, axis=1, keepdims=True) / DK
    spread = jnp.sum(totals * totals, axis=1, keepdims=True) / DK - center * center
    normed = (totals - center) * lax.rsqrt(spread + GN_EPS) * gn_gain_ref[:, own_head]
    gt_buf[me_kv] = pack(gate * normed)
    gt_copies = [to_kv(4, j, gt_buf.at[me_kv], gt_buf.at[me_kv]) for j in kv_order]

    loads["wo"].wait()
    for copy in gt_copies:
        copy.wait_recv()
    for c in range(n_kv):
        x_buf[:, pl.ds(c * DK, DK)] = unpack(gt_buf[c]).astype(BF16)
    o_buf[me_tp] = pack(jnp.dot(x_buf[...], wo[...], preferred_element_type=F32))
    o_copies = [to_tp(1, j, o_buf.at[me_tp], o_buf.at[me_tp]) for j in tp_order]
    for copy in o_copies:
        copy.wait_recv()
    squares = jnp.zeros((rows, 1), F32)
    mixed = unpack(o_buf[0])
    for t in range(1, n_tp):
        mixed = mixed + unpack(o_buf[t])
    for c in range(n_tp):
        cols = pl.ds(c * own_cols, own_cols)
        own_mixed = mixed[:, c * own_cols : (c + 1) * own_cols]
        resid = (tok_buf[c].astype(F32) + own_mixed).astype(BF16)
        resid_wide = resid.astype(F32)
        resid_buf[c] = resid_wide
        squares = squares + jnp.sum(resid_wide * resid_wide, axis=1, keepdims=True)
        x_buf[:, cols] = (resid_wide * ffn_gain_ref[:, cols]).astype(BF16)
    sqm_send[...] = jnp.broadcast_to(squares, (rows, LANES))
    sqm_copies = [to_kv(5, j, sqm_send, sqm_recv.at[j]) for j in kv_order]

    x = x_buf[...]
    loads["wfg"].wait()
    loads["wfu"].wait()
    gu_copies = []
    for j in kv_order + (0,):
        start = window_start(kv_peer(j), tiles, win // LANES, n_kv)
        cols = pl.ds(pl.multiple_of(start * LANES, LANES), win)
        gate = jnp.dot(x, wfg[:, cols], preferred_element_type=F32)
        up = jnp.dot(x, wfu[:, cols], preferred_element_type=F32)
        both = jnp.concatenate([gate, up], axis=0)
        if j:
            gu_send[j] = both.astype(BF16)
            gu_copies.append(to_kv(6, j, gu_send.at[j], gu_recv.at[j]))

    for copy in sqm_copies:
        copy.wait_recv()
    total_sq = sqm_send[...]
    for j in range(1, n_kv):
        total_sq = total_sq + sqm_recv[j]
    factor = lax.rsqrt(total_sq / D + RMS_EPS)[:, :1]
    for copy in gu_copies:
        copy.wait_recv()
    for j in kv_order:
        both = both + gu_recv[j].astype(F32)
    gate, up = both[:rows] * factor, both[rows:] * factor
    hidden = gate / (1.0 + jnp.exp(-gate)) * up
    here = window_start(me_kv, tiles, win // LANES, n_kv)
    after = window_start(me_kv + 1, tiles, win // LANES, n_kv)
    kept = jnp.where(me_kv == n_kv - 1, win, (after - here) * LANES)
    column = lax.broadcasted_iota(jnp.int32, (rows, win), 1)
    hid_buf[me_kv] = pack(jnp.where(column < kept, hidden, 0.0))
    hid_copies = [to_kv(7, j, hid_buf.at[me_kv], hid_buf.at[me_kv]) for j in kv_order]

    loads["wfd"].wait()
    down = None
    arrivals = dict(zip(kv_order, hid_copies))
    for j in range(n_kv):
        if j:
            arrivals[j].wait_recv()
        source = kv_peer(j)
        start = window_start(source, tiles, win // LANES, n_kv)
        weight = wfd[pl.ds(pl.multiple_of(start * LANES, LANES), win), :]
        chunk = unpack(hid_buf[source]).astype(BF16)
        part = jnp.dot(chunk, weight, preferred_element_type=F32)
        down = part if down is None else down + part
    down_buf[...] = down
    d_copies = {}
    for j in tp_order:
        cols = pl.ds(pl.multiple_of(tp_peer(j) * own_cols, own_cols), own_cols)
        d_send[j] = pack(down_buf[:, cols])
        d_copies[j] = to_tp(2, j, d_send.at[j], d_recv.at[j])
    own = pl.ds(pl.multiple_of(me_tp * own_cols, own_cols), own_cols)
    result = down_buf[:, own] + resid_buf[me_tp]
    for j in range(1, n_tp):
        d_copies[j].wait_recv()
        result = result + unpack(d_recv[j])
    out_ref[...] = result.astype(BF16)
    for copy in sent:
        copy.wait_send()


def fused(
    n_kv,
    n_tp,
    tokens,
    lengths,
    attn_gain,
    w_query,
    w_key,
    w_value,
    w_gate,
    log_decay,
    key_cache,
    value_cache,
    gn_gain,
    w_out,
    ffn_gain,
    w_ffn_gate,
    w_ffn_up,
    w_ffn_down,
):
    rows, own_cols = tokens.shape
    depth, wide = w_query.shape
    units = w_ffn_gate.shape[1]
    tiles = units // LANES
    win = -(-tiles // n_kv // 2) * 2 * LANES
    span = key_cache.shape[1]
    vmem = pl.BlockSpec(memory_space=pltpu.VMEM)
    smem = pl.BlockSpec(memory_space=pltpu.SMEM)
    hbm = pl.BlockSpec(memory_space=pl.ANY)
    streamed = (
        w_query,
        w_key,
        w_value,
        w_gate,
        key_cache,
        value_cache,
        w_out,
        w_ffn_gate,
        w_ffn_up,
        w_ffn_down,
    )
    scratch = [pltpu.VMEM(a.shape, a.dtype) for a in streamed] + [
        pltpu.VMEM((n_tp, rows, own_cols), BF16),
        pltpu.VMEM((rows, depth), BF16),
        pltpu.VMEM((rows, LANES), F32),
        pltpu.VMEM((n_kv, rows, LANES), F32),
        pltpu.VMEM((2 * rows, wide // 2), BF16),
        pltpu.VMEM((n_kv, 2 * rows, wide // 2), BF16),
        pltpu.VMEM((rows, wide), F32),
        pltpu.VMEM((2, rows, DK // 2), F32),
        pltpu.VMEM((n_kv, rows, rows * span), F32),
        pltpu.VMEM((n_kv, 2 * rows, 3 * DK // 2), BF16),
        pltpu.VMEM((n_kv, 2 * rows, 3 * DK // 2), BF16),
        pltpu.VMEM((rows, wide), F32),
        pltpu.VMEM((n_kv, 2 * rows, DK // 2), BF16),
        pltpu.VMEM((n_kv, 2 * rows, DK // 2), BF16),
        pltpu.VMEM((n_kv, 2 * rows, DK // 2), BF16),
        pltpu.VMEM((n_tp, 2 * rows, depth // 2), BF16),
        pltpu.VMEM((n_tp, rows, own_cols), F32),
        pltpu.VMEM((rows, LANES), F32),
        pltpu.VMEM((n_kv, rows, LANES), F32),
        pltpu.VMEM((n_kv, 2 * rows, win), BF16),
        pltpu.VMEM((n_kv, 2 * rows, win), BF16),
        pltpu.VMEM((n_kv, 2 * rows, win // 2), BF16),
        pltpu.VMEM((rows, depth), F32),
        pltpu.VMEM((n_tp, 2 * rows, own_cols // 2), BF16),
        pltpu.VMEM((n_tp, 2 * rows, own_cols // 2), BF16),
        pltpu.SemaphoreType.DMA((len(streamed),)),
        pltpu.SemaphoreType.DMA((8, n_kv)),
        pltpu.SemaphoreType.DMA((8, n_kv)),
        pltpu.SemaphoreType.DMA((3, n_tp)),
        pltpu.SemaphoreType.DMA((3, n_tp)),
    ]
    return pl.pallas_call(
        functools.partial(layer_kernel, n_kv, n_tp),
        out_shape=jax.ShapeDtypeStruct((rows, own_cols), BF16),
        in_specs=[vmem, smem, vmem, smem, vmem, vmem] + [hbm] * len(streamed),
        out_specs=vmem,
        scratch_shapes=scratch,
        compiler_params=pltpu.CompilerParams(
            collective_id=0, has_side_effects=True, vmem_limit_bytes=60 * 1024 * 1024
        ),
    )(
        tokens,
        lengths,
        attn_gain[None, :],
        log_decay,
        gn_gain[None, :],
        ffn_gain[None, :],
        *streamed,
    )


def fits(mesh, tokens, log_decay, key_cache, w_query, w_ffn_gate):
    n_kv, n_tp, n_grp = mesh.shape["kv"], mesh.shape["tp"], mesh.shape["grp"]
    heads, span = log_decay.shape[0], key_cache.shape[1] // n_kv
    return (
        n_kv > 1
        and n_tp > 1
        and n_kv & (n_kv - 1) == 0
        and n_tp & (n_tp - 1) == 0
        and heads == n_kv * n_tp
        and tokens.shape[1] // n_kv == heads * DK // n_tp
        and tokens.shape[1] % (n_kv * n_tp * 2 * LANES) == 0
        and w_ffn_gate.shape[1] % (n_tp * LANES) == 0
        and tokens.shape[0] // n_grp % 8 == 0
        and span % 16 == 0
        and span <= 64
    )


def solution(mesh):
    specs = (
        P("grp", ("kv", "tp")),
        P("grp"),
        P("kv"),
        P("kv", "tp"),
        P("kv", "tp"),
        P("kv", "tp"),
        P("kv", "tp"),
        P("tp"),
        P("grp", "kv", "tp"),
        P("grp", "kv", "tp"),
        P("tp"),
        P("tp", "kv"),
        P("kv"),
        P("kv", "tp"),
        P("kv", "tp"),
        P("tp", "kv"),
    )

    def whole(*arrays):
        tokens, w_query, log_decay, key_cache = arrays[0], arrays[3], arrays[7], arrays[8]
        if fits(mesh, tokens, log_decay, key_cache, w_query, arrays[13]):
            body = functools.partial(fused, mesh.shape["kv"], mesh.shape["tp"])
        else:
            body = local
        return jax.shard_map(
            body,
            mesh=mesh,
            in_specs=specs,
            out_specs=P("grp", ("kv", "tp")),
            check_vma=False,
        )(*arrays)

    return whole
```

```python
import functools
import math

import jax
import jax.numpy as jnp
from jax import lax
from jax.experimental import pallas as pl
from jax.experimental.pallas import tpu as pltpu
from jax.sharding import PartitionSpec as P

DK = 256
D = 4096


RMS_EPS = 0.1
GN_EPS = 1.0
ROPE_BASE = 10000.0


def rotate(vectors, positions):
    half_dim = vectors.shape[-1] // 2
    inverse = ROPE_BASE ** (-jnp.arange(half_dim, dtype=jnp.float32) / half_dim)
    angles = positions[:, None, None] * inverse[None, None, :]
    cosine = jnp.cos(angles)
    sine_part = jnp.sin(angles)
    front_part = vectors[..., :half_dim]
    back_part = vectors[..., half_dim:]
    return jnp.concatenate(
        [front_part * cosine - back_part * sine_part, front_part * sine_part + back_part * cosine],
        axis=-1,
    )


def group_norm(totals, gn_gain):
    width = totals.shape[-1]
    center = jnp.sum(totals, axis=-1, keepdims=True) / width
    spread = jnp.sum(totals * totals, axis=-1, keepdims=True) / width - center * center
    normed = (totals - center) * lax.rsqrt(spread + GN_EPS)
    return normed.reshape(normed.shape[0], -1) * gn_gain


def channel_stat(own_squares):
    return lax.psum(own_squares, "kv")


def input_stat(own_squares):
    return lax.psum(own_squares, "kv")


def cache_partial(query_low, lengths, log_decay, key_cache, value_cache, heads_here):
    batch_rows = query_low.shape[0]
    span = key_cache.shape[1]
    slots = lax.axis_index("kv") * span + jnp.arange(span, dtype=jnp.int32)
    live = slots[None, :] < lengths[:, None]
    gaps = jnp.maximum((lengths[:, None] - slots[None, :]).astype(jnp.float32), 0.0)
    decays = jnp.exp(log_decay[None, None, :] * gaps[:, :, None])
    keys_here = key_cache.reshape(batch_rows, span, heads_here, DK)
    values_here = value_cache.reshape(batch_rows, span, heads_here, DK)
    scores = jnp.einsum("bphd,bhd->bph", keys_here, query_low, preferred_element_type=jnp.float32)
    mixing = jnp.where(live[:, :, None], scores * decays, 0.0).astype(jnp.bfloat16)
    return jnp.einsum("bph,bphd->bhd", mixing, values_here, preferred_element_type=jnp.float32)


def local(
    tokens,
    lengths,
    attn_gain,
    w_query,
    w_key,
    w_value,
    w_gate,
    log_decay,
    key_cache,
    value_cache,
    gn_gain,
    w_out,
    ffn_gain,
    w_ffn_gate,
    w_ffn_up,
    w_ffn_down,
):
    batch_rows = tokens.shape[0]
    heads_here = log_decay.shape[0]
    row_block = lax.all_gather(tokens, "tp", axis=1, tiled=True)
    widened = row_block.astype(jnp.float32)
    own_squares = jnp.sum(widened * widened, axis=1)
    scaled = (widened * attn_gain).astype(jnp.bfloat16)
    part_query = jnp.dot(scaled, w_query, preferred_element_type=jnp.float32)
    part_key = jnp.dot(scaled, w_key, preferred_element_type=jnp.float32)
    part_value = jnp.dot(scaled, w_value, preferred_element_type=jnp.float32)
    part_gate = jnp.dot(scaled, w_gate, preferred_element_type=jnp.float32)
    positions = lengths.astype(jnp.float32)
    total_squares = input_stat(own_squares)
    queries, new_keys, new_values, gates = lax.psum(
        (part_query, part_key, part_value, part_gate), "kv"
    )
    factor = lax.rsqrt(total_squares / D + RMS_EPS)[:, None]
    queries = rotate((queries * factor).reshape(batch_rows, heads_here, DK), positions) * DK ** (
        -0.5
    )
    new_keys = rotate((new_keys * factor).reshape(batch_rows, heads_here, DK), positions)
    new_values = (new_values * factor).reshape(batch_rows, heads_here, DK)
    gates = gates * factor
    query_low = queries.astype(jnp.bfloat16)
    partial_value = cache_partial(query_low, lengths, log_decay, key_cache, value_cache, heads_here)
    cached = lax.psum(partial_value.reshape(batch_rows, heads_here * DK), "kv")
    own_term = jnp.sum(queries * new_keys, axis=-1, keepdims=True) * new_values
    normed = group_norm(cached.reshape(batch_rows, heads_here, DK) + own_term, gn_gain)
    gated = (jax.nn.silu(gates) * normed).astype(jnp.bfloat16)
    out_partial = jnp.dot(gated, w_out, preferred_element_type=jnp.float32)
    mixed = lax.psum_scatter(out_partial, "tp", scatter_dimension=1, tiled=True)
    resid = (tokens.astype(jnp.float32) + mixed).astype(jnp.bfloat16)
    resid_block = lax.all_gather(resid, "tp", axis=1, tiled=True).astype(jnp.float32)
    mid_squares = jnp.sum(resid_block * resid_block, axis=1)
    scaled_mid = (resid_block * ffn_gain).astype(jnp.bfloat16)
    gate_part = jnp.dot(scaled_mid, w_ffn_gate, preferred_element_type=jnp.float32)
    up_part = jnp.dot(scaled_mid, w_ffn_up, preferred_element_type=jnp.float32)
    total_mid = channel_stat(mid_squares)
    gate_sum, up_sum = lax.psum((gate_part, up_part), "kv")
    factor_mid = lax.rsqrt(total_mid / D + RMS_EPS)[:, None]
    hidden = (jax.nn.silu(gate_sum * factor_mid) * (up_sum * factor_mid)).astype(jnp.bfloat16)
    down_partial = jnp.dot(hidden, w_ffn_down, preferred_element_type=jnp.float32)
    down = lax.psum_scatter(down_partial, "tp", scatter_dimension=1, tiled=True)
    return (resid.astype(jnp.float32) + down).astype(jnp.bfloat16)


LANES = 128
F32 = jnp.float32
BF16 = jnp.bfloat16


def window_start(index, tiles, width, parts):
    return (index * (tiles - width) + (parts - 1) // 2) // (parts - 1)


def partner(index, j, parts):
    found, bit = 0, 1
    while bit < parts:
        digit = (index // bit) % 2
        found = found + bit * ((1 - digit) if (j // bit) % 2 else digit)
        bit *= 2
    return found


def pack(value):
    middle = value.shape[1] // 2
    return jnp.concatenate([value[:, :middle], value[:, middle:]], axis=0).astype(BF16)


def unpack(packed):
    wide = packed.astype(F32)
    rows = wide.shape[0] // 2
    return jnp.concatenate([wide[:rows], wide[rows:]], axis=1)


def layer_kernel(
    n_kv,
    n_tp,
    tokens_ref,
    lengths_ref,
    attn_gain_ref,
    log_decay_ref,
    gn_gain_ref,
    ffn_gain_ref,
    wq_hbm,
    wk_hbm,
    wv_hbm,
    wg_hbm,
    kc_hbm,
    vc_hbm,
    wo_hbm,
    wfg_hbm,
    wfu_hbm,
    wfd_hbm,
    out_ref,
    wq,
    wk,
    wv,
    wg,
    kc,
    vc,
    wo,
    wfg,
    wfu,
    wfd,
    tok_buf,
    x_buf,
    sq_send,
    sq_recv,
    q_send,
    q_recv,
    q_full,
    trig,
    decay_buf,
    kvg_send,
    kvg_recv,
    ca_send,
    ca_recv,
    gt_buf,
    o_buf,
    resid_buf,
    sqm_send,
    sqm_recv,
    gu_send,
    gu_recv,
    hid_buf,
    down_buf,
    d_send,
    d_recv,
    load_sem,
    kv_send_sem,
    kv_recv_sem,
    tp_send_sem,
    tp_recv_sem,
):
    rows, own_cols = tokens_ref.shape
    depth, wide = wq.shape
    span = kc.shape[1]
    half = DK // 2
    tiles = wfg.shape[1] // LANES
    win = gu_send.shape[3] * 2
    me_kv = lax.axis_index("kv")
    me_tp = lax.axis_index("tp")

    def kv_peer(j):
        return partner(me_kv, j, n_kv)

    def tp_peer(j):
        return partner(me_tp, j, n_tp)

    kv_order = tuple(range(n_kv - 1, 0, -1))
    tp_order = tuple(range(n_tp - 1, 0, -1))

    loads = {}
    for slot, (name, src, dst) in enumerate(
        (
            ("wq", wq_hbm, wq),
            ("kc", kc_hbm, kc),
            ("vc", vc_hbm, vc),
            ("wk", wk_hbm, wk),
            ("wv", wv_hbm, wv),
            ("wg", wg_hbm, wg),
            ("wo", wo_hbm, wo),
            ("wfg", wfg_hbm, wfg),
            ("wfu", wfu_hbm, wfu),
            ("wfd", wfd_hbm, wfd),
        )
    ):
        loads[name] = pltpu.make_async_copy(src, dst, load_sem.at[slot])

    sent = []

    def to_kv(phase, j, src, dst):
        copy = pltpu.make_async_remote_copy(
            src_ref=src,
            dst_ref=dst,
            send_sem=kv_send_sem.at[phase, j],
            recv_sem=kv_recv_sem.at[phase, j],
            device_id={"kv": kv_peer(j)},
            device_id_type=pl.DeviceIdType.MESH,
        )
        copy.start()
        sent.append(copy)
        return copy

    def to_tp(phase, j, src, dst):
        copy = pltpu.make_async_remote_copy(
            src_ref=src,
            dst_ref=dst,
            send_sem=tp_send_sem.at[phase, j],
            recv_sem=tp_recv_sem.at[phase, j],
            device_id={"tp": tp_peer(j)},
            device_id_type=pl.DeviceIdType.MESH,
        )
        copy.start()
        sent.append(copy)
        return copy

    loads["wq"].start()

    barrier = pltpu.get_barrier_semaphore()
    for j in range(1, n_kv):
        pl.semaphore_signal(
            barrier, inc=1, device_id={"kv": kv_peer(j)}, device_id_type=pl.DeviceIdType.MESH
        )
    for j in range(1, n_tp):
        pl.semaphore_signal(
            barrier, inc=1, device_id={"tp": tp_peer(j)}, device_id_type=pl.DeviceIdType.MESH
        )
    pl.semaphore_wait(barrier, n_kv + n_tp - 2)

    tok_copies = [to_tp(0, j, tokens_ref, tok_buf.at[me_tp]) for j in tp_order]
    for name in ("wk", "wv", "wg", "kc", "vc"):
        loads[name].start()
    tok_buf[me_tp] = tokens_ref[...]

    row_id = lax.broadcasted_iota(jnp.int32, (rows, LANES), 0)
    lens = jnp.zeros((rows, LANES), jnp.int32)
    for b in range(rows):
        lens = jnp.where(row_id == b, lengths_ref[b], lens)
    lane = lax.broadcasted_iota(jnp.int32, (rows, half), 1).astype(F32)
    inverse = jnp.exp(lane * (-math.log(ROPE_BASE) / half))
    angles = lens[:, :1].astype(F32) * inverse
    trig[0] = jnp.cos(angles)
    trig[1] = jnp.sin(angles)
    places = rows * span
    col = lax.broadcasted_iota(jnp.int32, (rows, places), 1)
    row = lax.broadcasted_iota(jnp.int32, (rows, places), 0)
    slot = col - row * span
    position = slot + me_kv * span
    gap = lens[:, :1] - position
    live = (slot >= 0) & (slot < span) & (gap > 0)
    gap_f = jnp.where(live, gap, 0).astype(F32)
    for h in range(n_kv):
        decay_buf[h] = jnp.where(live, jnp.exp(gap_f * log_decay_ref[h]), 0.0)

    def rotate_in(front, back):
        cosine, sine = trig[0], trig[1]
        return front * cosine - back * sine, front * sine + back * cosine

    for copy in tok_copies:
        copy.wait_recv()
    squares = jnp.zeros((rows, 1), F32)
    for c in range(n_tp):
        wide_tok = tok_buf[c].astype(F32)
        squares = squares + jnp.sum(wide_tok * wide_tok, axis=1, keepdims=True)
        cols = pl.ds(c * own_cols, own_cols)
        x_buf[:, cols] = (wide_tok * attn_gain_ref[:, cols]).astype(BF16)
    sq_send[...] = jnp.broadcast_to(squares, (rows, LANES))
    sq_copies = [to_kv(0, j, sq_send, sq_recv.at[j]) for j in kv_order]

    x = x_buf[...]
    loads["wq"].wait()
    q_copies = []
    for part in range(2):
        cols = pl.ds(part * (wide // 2), wide // 2)
        q_own = jnp.dot(x, wq[:, cols], preferred_element_type=F32)
        q_send[part] = pack(q_own)
        q_full[:, cols] = q_own
        for j in kv_order:
            q_copies.append(to_kv(1 + 7 * part, j, q_send.at[part], q_recv.at[part, j]))
    for name in ("wo", "wfg", "wfu", "wfd"):
        loads[name].start()

    for name in ("wk", "wv", "wg"):
        loads[name].wait()
    kvg_copies = []
    for j in kv_order + (0,):
        cols = pl.ds(pl.multiple_of(kv_peer(j) * DK, DK), DK)
        parts = [
            jnp.dot(x, weight[:, cols], preferred_element_type=F32) for weight in (wk, wv, wg)
        ]
        if j:
            kvg_send[j] = pack(jnp.concatenate(parts, axis=1))
            kvg_copies.append(to_kv(2, j, kvg_send.at[j], kvg_recv.at[j]))
        else:
            own_kvg = jnp.concatenate(parts, axis=1)

    for copy in sq_copies:
        copy.wait_recv()
    total_sq = sq_send[...]
    for j in range(1, n_kv):
        total_sq = total_sq + sq_recv[j]
    factor = lax.rsqrt(total_sq / D + RMS_EPS)[:, :1]

    loads["kc"].wait()
    loads["vc"].wait()
    for copy in q_copies:
        copy.wait_recv()
    parts = []
    for part in range(2):
        piece = q_full[:, pl.ds(part * (wide // 2), wide // 2)]
        for j in kv_order:
            piece = piece + unpack(q_recv[part, j])
        parts.append(piece * factor)
    query = jnp.concatenate(parts, axis=1)
    for h in range(n_kv):
        halves = (query[:, h * DK : h * DK + half], query[:, h * DK + half : (h + 1) * DK])
        front, back = rotate_in(*halves)
        q_full[:, pl.ds(h * DK, half)] = front * DK ** (-0.5)
        q_full[:, pl.ds(h * DK + half, half)] = back * DK ** (-0.5)
    ca_copies = []
    for j in kv_order + (0,):
        head = kv_peer(j)
        cols = pl.ds(pl.multiple_of(head * DK, DK), DK)
        keys = kc[:, :, cols].reshape(places, DK)
        scores = lax.dot_general(
            q_full[:, cols].astype(BF16),
            keys,
            (((1,), (1,)), ((), ())),
            preferred_element_type=F32,
        )
        mixing = (scores * decay_buf[head]).astype(BF16)
        values = vc[:, :, cols].reshape(places, DK)
        cached = jnp.dot(mixing, values, preferred_element_type=F32)
        if j:
            ca_send[j] = pack(cached)
            ca_copies.append(to_kv(3, j, ca_send.at[j], ca_recv.at[j]))

    for copy in kvg_copies:
        copy.wait_recv()
    own_head = pl.ds(pl.multiple_of(me_kv * DK, DK), DK)
    for j in kv_order:
        own_kvg = own_kvg + unpack(kvg_recv[j])
    own_kvg = own_kvg * factor
    summed = [own_kvg[:, i * DK : (i + 1) * DK] for i in range(3)]
    new_key, new_value, gate = summed
    front, back = rotate_in(new_key[:, :half], new_key[:, half:])
    query = q_full[:, own_head]
    score = jnp.sum(query[:, :half] * front + query[:, half:] * back, axis=1, keepdims=True)
    own_term = score * new_value
    gate = gate / (1.0 + jnp.exp(-gate))
    totals = own_term + cached
    for copy in ca_copies:
        copy.wait_recv()
    for j in range(1, n_kv):
        totals = totals + unpack(ca_recv[j])
    center = jnp.sum(totals, axis=1, keepdims=True) / DK
    spread = jnp.sum(totals * totals, axis=1, keepdims=True) / DK - center * center
    normed = (totals - center) * lax.rsqrt(spread + GN_EPS) * gn_gain_ref[:, own_head]
    gt_buf[me_kv] = pack(gate * normed)
    gt_copies = [to_kv(4, j, gt_buf.at[me_kv], gt_buf.at[me_kv]) for j in kv_order]

    loads["wo"].wait()
    for copy in gt_copies:
        copy.wait_recv()
    for c in range(n_kv):
        x_buf[:, pl.ds(c * DK, DK)] = unpack(gt_buf[c]).astype(BF16)
    o_buf[me_tp] = pack(jnp.dot(x_buf[...], wo[...], preferred_element_type=F32))
    o_copies = [to_tp(1, j, o_buf.at[me_tp], o_buf.at[me_tp]) for j in tp_order]
    for copy in o_copies:
        copy.wait_recv()
    squares = jnp.zeros((rows, 1), F32)
    mixed = unpack(o_buf[0])
    for t in range(1, n_tp):
        mixed = mixed + unpack(o_buf[t])
    for c in range(n_tp):
        cols = pl.ds(c * own_cols, own_cols)
        own_mixed = mixed[:, c * own_cols : (c + 1) * own_cols]
        resid = (tok_buf[c].astype(F32) + own_mixed).astype(BF16)
        resid_wide = resid.astype(F32)
        resid_buf[c] = resid_wide
        squares = squares + jnp.sum(resid_wide * resid_wide, axis=1, keepdims=True)
        x_buf[:, cols] = (resid_wide * ffn_gain_ref[:, cols]).astype(BF16)
    sqm_send[...] = jnp.broadcast_to(squares, (rows, LANES))
    sqm_copies = [to_kv(5, j, sqm_send, sqm_recv.at[j]) for j in kv_order]

    x = x_buf[...]
    loads["wfg"].wait()
    loads["wfu"].wait()
    gu_copies = []
    for j in kv_order + (0,):
        start = window_start(kv_peer(j), tiles, win // LANES, n_kv)
        cols = pl.ds(pl.multiple_of(start * LANES, LANES), win)
        both = []
        for i, weight in enumerate((wfg, wfu)):
            part = jnp.dot(x, weight[:, cols], preferred_element_type=F32)
            both.append(part)
            if j:
                gu_send[i, j] = pack(part)
                gu_copies.append(to_kv(6 + 3 * i, j, gu_send.at[i, j], gu_recv.at[i, j]))

    for copy in sqm_copies:
        copy.wait_recv()
    total_sq = sqm_send[...]
    for j in range(1, n_kv):
        total_sq = total_sq + sqm_recv[j]
    factor = lax.rsqrt(total_sq / D + RMS_EPS)[:, :1]
    for copy in gu_copies:
        copy.wait_recv()
    for i in range(2):
        for j in kv_order:
            both[i] = both[i] + unpack(gu_recv[i, j])
    gate, up = both[0] * factor, both[1] * factor
    hidden = gate / (1.0 + jnp.exp(-gate)) * up
    here = window_start(me_kv, tiles, win // LANES, n_kv)
    after = window_start(me_kv + 1, tiles, win // LANES, n_kv)
    kept = jnp.where(me_kv == n_kv - 1, win, (after - here) * LANES)
    column = lax.broadcasted_iota(jnp.int32, (rows, win), 1)
    hid_buf[me_kv] = pack(jnp.where(column < kept, hidden, 0.0))
    hid_copies = [to_kv(7, j, hid_buf.at[me_kv], hid_buf.at[me_kv]) for j in kv_order]

    loads["wfd"].wait()
    down = None
    arrivals = dict(zip(kv_order, hid_copies))
    for j in range(n_kv):
        if j:
            arrivals[j].wait_recv()
        source = kv_peer(j)
        start = window_start(source, tiles, win // LANES, n_kv)
        weight = wfd[pl.ds(pl.multiple_of(start * LANES, LANES), win), :]
        chunk = unpack(hid_buf[source]).astype(BF16)
        part = jnp.dot(chunk, weight, preferred_element_type=F32)
        down = part if down is None else down + part
    down_buf[...] = down
    d_copies = {}
    for j in tp_order:
        cols = pl.ds(pl.multiple_of(tp_peer(j) * own_cols, own_cols), own_cols)
        d_send[j] = pack(down_buf[:, cols])
        d_copies[j] = to_tp(2, j, d_send.at[j], d_recv.at[j])
    own = pl.ds(pl.multiple_of(me_tp * own_cols, own_cols), own_cols)
    result = down_buf[:, own] + resid_buf[me_tp]
    for j in range(1, n_tp):
        d_copies[j].wait_recv()
        result = result + unpack(d_recv[j])
    out_ref[...] = result.astype(BF16)
    for copy in sent:
        copy.wait_send()


def fused(
    n_kv,
    n_tp,
    tokens,
    lengths,
    attn_gain,
    w_query,
    w_key,
    w_value,
    w_gate,
    log_decay,
    key_cache,
    value_cache,
    gn_gain,
    w_out,
    ffn_gain,
    w_ffn_gate,
    w_ffn_up,
    w_ffn_down,
):
    rows, own_cols = tokens.shape
    depth, wide = w_query.shape
    units = w_ffn_gate.shape[1]
    tiles = units // LANES
    win = -(-tiles // n_kv // 2) * 2 * LANES
    span = key_cache.shape[1]
    vmem = pl.BlockSpec(memory_space=pltpu.VMEM)
    smem = pl.BlockSpec(memory_space=pltpu.SMEM)
    hbm = pl.BlockSpec(memory_space=pl.ANY)
    streamed = (
        w_query,
        w_key,
        w_value,
        w_gate,
        key_cache,
        value_cache,
        w_out,
        w_ffn_gate,
        w_ffn_up,
        w_ffn_down,
    )
    scratch = [pltpu.VMEM(a.shape, a.dtype) for a in streamed] + [
        pltpu.VMEM((n_tp, rows, own_cols), BF16),
        pltpu.VMEM((rows, depth), BF16),
        pltpu.VMEM((rows, LANES), F32),
        pltpu.VMEM((n_kv, rows, LANES), F32),
        pltpu.VMEM((2, 2 * rows, wide // 4), BF16),
        pltpu.VMEM((2, n_kv, 2 * rows, wide // 4), BF16),
        pltpu.VMEM((rows, wide), F32),
        pltpu.VMEM((2, rows, DK // 2), F32),
        pltpu.VMEM((n_kv, rows, rows * span), F32),
        pltpu.VMEM((n_kv, 2 * rows, 3 * DK // 2), BF16),
        pltpu.VMEM((n_kv, 2 * rows, 3 * DK // 2), BF16),
        pltpu.VMEM((n_kv, 2 * rows, DK // 2), BF16),
        pltpu.VMEM((n_kv, 2 * rows, DK // 2), BF16),
        pltpu.VMEM((n_kv, 2 * rows, DK // 2), BF16),
        pltpu.VMEM((n_tp, 2 * rows, depth // 2), BF16),
        pltpu.VMEM((n_tp, rows, own_cols), F32),
        pltpu.VMEM((rows, LANES), F32),
        pltpu.VMEM((n_kv, rows, LANES), F32),
        pltpu.VMEM((2, n_kv, 2 * rows, win // 2), BF16),
        pltpu.VMEM((2, n_kv, 2 * rows, win // 2), BF16),
        pltpu.VMEM((n_kv, 2 * rows, win // 2), BF16),
        pltpu.VMEM((rows, depth), F32),
        pltpu.VMEM((n_tp, 2 * rows, own_cols // 2), BF16),
        pltpu.VMEM((n_tp, 2 * rows, own_cols // 2), BF16),
        pltpu.SemaphoreType.DMA((len(streamed),)),
        pltpu.SemaphoreType.DMA((10, n_kv)),
        pltpu.SemaphoreType.DMA((10, n_kv)),
        pltpu.SemaphoreType.DMA((3, n_tp)),
        pltpu.SemaphoreType.DMA((3, n_tp)),
    ]
    return pl.pallas_call(
        functools.partial(layer_kernel, n_kv, n_tp),
        out_shape=pltpu.VMEM((rows, own_cols), BF16),
        in_specs=[vmem, smem, vmem, smem, vmem, vmem] + [hbm] * len(streamed),
        out_specs=vmem,
        scratch_shapes=scratch,
        compiler_params=pltpu.CompilerParams(
            collective_id=0, has_side_effects=True, vmem_limit_bytes=60 * 1024 * 1024
        ),
    )(
        tokens,
        lengths,
        attn_gain[None, :],
        log_decay,
        gn_gain[None, :],
        ffn_gain[None, :],
        *streamed,
    )


def fits(mesh, tokens, log_decay, key_cache, w_query, w_ffn_gate):
    n_kv, n_tp, n_grp = mesh.shape["kv"], mesh.shape["tp"], mesh.shape["grp"]
    heads, span = log_decay.shape[0], key_cache.shape[1] // n_kv
    return (
        n_kv > 1
        and n_tp > 1
        and n_kv & (n_kv - 1) == 0
        and n_tp & (n_tp - 1) == 0
        and heads == n_kv * n_tp
        and tokens.shape[1] // n_kv == heads * DK // n_tp
        and tokens.shape[1] % (n_kv * n_tp * 2 * LANES) == 0
        and heads * DK // n_tp % (4 * LANES) == 0
        and w_ffn_gate.shape[1] % (n_tp * LANES) == 0
        and tokens.shape[0] // n_grp % 8 == 0
        and span % 16 == 0
        and span <= 64
    )


def solution(mesh):
    specs = (
        P("grp", ("kv", "tp")),
        P("grp"),
        P("kv"),
        P("kv", "tp"),
        P("kv", "tp"),
        P("kv", "tp"),
        P("kv", "tp"),
        P("tp"),
        P("grp", "kv", "tp"),
        P("grp", "kv", "tp"),
        P("tp"),
        P("tp", "kv"),
        P("kv"),
        P("kv", "tp"),
        P("kv", "tp"),
        P("tp", "kv"),
    )

    def whole(*arrays):
        tokens, w_query, log_decay, key_cache = arrays[0], arrays[3], arrays[7], arrays[8]
        if fits(mesh, tokens, log_decay, key_cache, w_query, arrays[13]):
            body = functools.partial(fused, mesh.shape["kv"], mesh.shape["tp"])
        else:
            body = local
        return jax.shard_map(
            body,
            mesh=mesh,
            in_specs=specs,
            out_specs=P("grp", ("kv", "tp")),
            check_vma=False,
        )(*arrays)

    return whole
```
